32 devices in a mesh: sp: 8 (over z, core), tp: 4 (over y, x).
Axes of the slice: x: 2, y: 2, z: 4, core: 2. Of those that a mesh axis runs over, the one named last changes fastest.
Arguments:
- skip_path_vectors: bfloat16 [2048, 2048], P('sp'), may hold values from -10 to 10
- asker_raw_scores: bfloat16 [2048, 2048], P('sp', 'tp'), may hold values from -6 to 6
- retain_raw_scores: bfloat16 [2048, 2048], P('sp', 'tp'), may hold values from -5.5 to 5.5
- memory_write_entries: bfloat16 [2048, 2048], P('sp', 'tp'), may hold values from -6 to 6
- emit_switch_scores: bfloat16 [2048, 2048], P('sp', 'tp'), may hold values from -6 to 6
- retain_minimum_share: float32 [2048], P('tp'), may hold values from 0.88 to 0.99990234
- extra_shrink_rate: float32 [16, 2048], P('tp', 'sp'), may hold values from -0.7 to 0
- lane_rescale_factor: float32 [128], replicated, may hold values from 0.1 to 1.9
- emit_projection_array: bfloat16 [2048, 2048], P('tp'), may hold values from -0.1875 to 0.1875
- specialist_rescale_factor: float32 [2048], replicated, may hold values from 0.1 to 1.9
- specialist_switch_proj: bfloat16 [8, 2048, 4096], P('sp', None, 'tp'), may hold values from -0.125 to 0.125
- specialist_raise_proj: bfloat16 [8, 2048, 4096], P('sp', None, 'tp'), may hold values from -0.125 to 0.125
- specialist_lower_proj: bfloat16 [8, 4096, 2048], P('sp', 'tp'), may hold values from -0.375 to 0.375
- specialist_choice_ids: int32 [2048, 2], P('sp'), may hold values from 0 to 7, all different within a row; in each aligned block of 256 rows (0 to 255, 256 to 511, ...) at most 96 rows name the same one
- cluster_chance: float32 [2048], P('sp'), may hold values from 0.1 to 0.6
- specialist_duo_scores: float32 [2048, 2], P('sp'), may hold values from -2 to 2
Outputs:
- mixed_out: bfloat16 [2048, 2048], P('sp', 'tp')
The draws below stay inside these ranges and needn't reach their ends.
Inputs may be any that keep to these rules, and one draw needn't show every extreme that they name: `specialist_choice_ids`: in each aligned block of 256 rows (the rows of one index of sp) no expert is named by more than 96 rows, a bound that some block reaches; the 2 ids of a row differ.
All inputs are finite; a program needn't handle non-finite values.
Results may differ from the reference program's by a relative error of at most 0.02.
Values may be sent and summed in bfloat16 or wider, within the bound.
A program may use at most 64 MiB of HBM per device.

```python
import math
import jax
import jax.numpy as jnp
import numpy as np
from jax import lax

D = 2048
SCAN_LANE_COUNT = 16
KEY_WIDTH_SIZE = 128
FFE = 4096
TOPK = 2
TOK_SP = 256
HG_W = 2048
EXPERTS = 8
SEQ = 2048
CAP = 96
N_SP = 8
N_TP = 4


def draw_skip_path_vectors(key, part):
    noise_key, row_key = jax.random.split(key)
    columns = jnp.arange(D, dtype=jnp.float32) / D
    noise = jnp.clip(jax.random.normal(noise_key, (SEQ, D), jnp.float32), -3.0, 3.0)
    col_scale = 10.0 ** (columns - 0.5)
    row_scale = 0.3 * jnp.exp(jax.random.uniform(row_key, (SEQ,), jnp.float32, math.log(0.3), math.log(3.0)))
    return (noise * row_scale[:, None] * col_scale[None, :]).astype(jnp.bfloat16)


def draw_retain_raw_scores(key, part):
    noise_key, shift_key = jax.random.split(key)
    blocks = SEQ // TOK_SP
    noise = jnp.clip(jax.random.normal(noise_key, (SEQ, HG_W), jnp.float32), -4.0, 4.0)
    shifts = jax.random.uniform(shift_key, (blocks, 1, 1), jnp.float32, -1.0, 1.0)
    return (noise.reshape(blocks, TOK_SP, HG_W) + shifts).reshape(SEQ, HG_W).astype(jnp.bfloat16)


def draw_retain_minimum_share(key, part):
    pick_key, slow_key, fast_key = jax.random.split(key, 3)
    slow_head = jax.random.randint(pick_key, (SCAN_LANE_COUNT,), 0, 2) > 0
    slow_gap = jnp.exp(jax.random.uniform(slow_key, (SCAN_LANE_COUNT, KEY_WIDTH_SIZE), jnp.float32, math.log(0.2), math.log(1.2))) / SEQ
    fast_gap = jnp.exp(jax.random.uniform(fast_key, (SCAN_LANE_COUNT, KEY_WIDTH_SIZE), jnp.float32, math.log(0.04), math.log(0.12)))
    gap = jnp.where(slow_head[:, None], slow_gap, fast_gap)
    return (1.0 - gap).reshape(HG_W).astype(jnp.float32)


def draw_extra_shrink_rate(key, part):
    where_key, size_key = jax.random.split(key)
    spots = jax.random.randint(where_key, (3,), 0, SEQ)
    strength = jnp.log(jax.random.uniform(size_key, (SCAN_LANE_COUNT, 3), jnp.float32, 0.5, 0.8))
    places = jnp.arange(SEQ)[None, None, :] == spots[None, :, None]
    return jnp.sum(jnp.where(places, strength[:, :, None], 0.0), axis=1).astype(jnp.float32)


def with_spikes(values, rng, source, target, blocks, factor):
    def block_of(position):
        return (jnp.arange(values.shape[position]) // (values.shape[position] // blocks)).reshape((-1,) + (1,) * (values.ndim - 1 - position))

    near = jax.random.permutation(rng, blocks)[block_of(target)]
    other_side = (block_of(target) + blocks // 2) % blocks
    return jnp.where((block_of(source) == near) | (block_of(source) == other_side), factor * values, values)


def steps_of(stream_key, dims, cuts, low, largest):
    gain, own = 1.0, jax.random.fold_in(stream_key, 6)
    for axis_at, parts in cuts:
        steps = jnp.exp(jax.random.uniform(jax.random.fold_in(own, axis_at), (parts,), jnp.float32, low / len(cuts), largest / len(cuts)))
        gain = gain * jnp.repeat(steps, dims[axis_at] // parts).reshape([-1 if axis == axis_at else 1 for axis in range(len(dims))])
    return gain


def routed_block(rng, own, number, rows, count, top, limit, skew):
    ranking = jax.random.permutation(rng, count)
    crowded, ordinary = shares(count, rows * top, limit, skew, True), shares(count, rows * top, limit, skew, False)
    places = jnp.arange(count)

    def named(sizes, rotation):
        used = int((sizes > 0).sum())
        fixed = max(1, used // 4)
        shifted = fixed + (places - fixed + rotation * (used - fixed)) % max(1, count - fixed)
        return jnp.zeros((count,), jnp.int32).at[ranking[jnp.where(places < fixed, places, shifted)]].set(jnp.asarray(sizes, jnp.int32))

    sizes = jnp.where(number % 4 == 0, named(crowded, number // 4), named(ordinary, number - number // 4 - 1))
    mixed = jax.random.permutation(jax.random.fold_in(own, 3), count)
    source_of, taker = mixed[0:count // 2 * 2:2], mixed[1:count // 2 * 2:2]
    margin = jnp.minimum(sizes[source_of] - 1, limit - sizes[taker]) // 2
    margin = jnp.where((source_of == ranking[0]) | (taker == ranking[0]) | (sizes[taker] == 0), 0, jnp.maximum(margin, 0))
    shifted = jax.random.randint(jax.random.fold_in(own, 4), (count // 2,), 0, 1 << 20) % (margin + 1)
    sizes = sizes.at[source_of].add(-shifted).at[taker].add(shifted)
    labels = jnp.searchsorted(jnp.cumsum(sizes), jnp.arange(rows * top), side="right").astype(jnp.int32)
    grid = labels.reshape(top, rows).T
    grid = grid[jax.random.permutation(jax.random.fold_in(own, 1), rows)]
    rotation = jax.random.randint(jax.random.fold_in(own, 2), (rows, 1), 0, top)
    return jnp.take_along_axis(grid, (jnp.arange(top)[None, :] + rotation) % top, axis=1)


def shares(amount, total, bound, slope, full):
    weights = [(1 << 20) // math.isqrt(standing ** slope) + 1 for standing in range(1, amount + 1)]
    largest = bound if full else min(bound, max(-(-total // amount), total * weights[0] // sum(weights)))
    least = 1 if total - largest >= amount - 1 else 0
    holding, surplus = [largest] + [least] * (amount - 1), total - largest - least * (amount - 1)
    while surplus > 0:
        candidates = [i for i in range(1, amount) if holding[i] < largest] or [i for i in range(1, amount) if holding[i] < bound]
        mass, remaining = sum([weights[i] for i in candidates]), surplus
        for i in candidates:
            addition = min(bound - holding[i], max(1, remaining * weights[i] // mass), surplus)
            holding[i] = holding[i] + addition
            surplus = surplus - addition
    return np.array(holding)


def scatter_about(rng, shape, width, most, shards=(), held_as=jnp.bfloat16):
    loudness = steps_of(rng, shape, shards, -0.22, 0.18) if shards else 1.0
    entries = jax.random.normal(rng, shape, jnp.float32) * width * loudness
    return jnp.minimum(jnp.maximum(entries, -most), most).astype(held_as)


def bell_draw_with(rng, shape, width, limit, pieces, heavy, kind=jnp.bfloat16):
    values = width * jax.random.normal(rng, shape, jnp.float32)
    if pieces:
        values = values * steps_of(rng, shape, pieces, -0.22, 0.18)
    return jnp.clip(with_spikes(values, jax.random.fold_in(rng, 3), *heavy), -limit, limit).astype(kind)


def setup_inputs(seed: int = 0) -> dict:
    streams_of = jax.random.split(jax.random.key(seed), 17)
    skip_path_vectors = draw_skip_path_vectors(jax.random.fold_in(streams_of[16], 71), 0)
    asker_raw_scores = scatter_about(streams_of[1], (SEQ, HG_W), 1.0, 6.0, ((0, 8), (1, 4)))
    retain_raw_scores = draw_retain_raw_scores(jax.random.fold_in(streams_of[16], 71), 0)
    memory_write_entries = scatter_about(streams_of[3], (SEQ, HG_W), 1.0, 6.0, ((0, 8), (1, 4)))
    emit_switch_scores = scatter_about(streams_of[4], (SEQ, HG_W), 1.0, 6.0, ((0, 8), (1, 4)))
    retain_minimum_share = draw_retain_minimum_share(jax.random.fold_in(streams_of[16], 71), 0)
    extra_shrink_rate = draw_extra_shrink_rate(jax.random.fold_in(streams_of[16], 71), 0)
    lane_rescale_factor = jnp.clip(1.0 + 0.18 * jax.random.normal(streams_of[7], (KEY_WIDTH_SIZE,), jnp.float32), 0.1, 1.9)
    emit_projection_array = bell_draw_with(streams_of[8], (HG_W, D), HG_W ** -0.5, 0.1875, ((0, 4),), (0, 1, 4, 2.0))
    specialist_rescale_factor = jnp.clip(1.0 + 0.18 * jax.random.normal(streams_of[9], (D,), jnp.float32), 0.1, 1.9)
    specialist_switch_proj = scatter_about(streams_of[10], (EXPERTS, D, FFE), D ** -0.5, 0.125, ((0, 8), (2, 4)))
    specialist_raise_proj = scatter_about(streams_of[11], (EXPERTS, D, FFE), D ** -0.5, 0.125, ((0, 8), (2, 4)))
    specialist_lower_proj = bell_draw_with(streams_of[12], (EXPERTS, FFE, D), (FFE // 8) ** -0.5, 0.375, ((0, 8), (1, 4)), (1, 2, 4, 2.0))
    specialist_choice_ids_keys = jax.random.split(jax.random.fold_in(streams_of[13], 1), SEQ // TOK_SP)
    specialist_choice_ids_turns = jax.random.permutation(jax.random.fold_in(streams_of[13], 3), SEQ // TOK_SP)
    specialist_choice_ids = jax.vmap(lambda own, number: routed_block(jax.random.fold_in(streams_of[13], 2), own, number, TOK_SP, EXPERTS, TOPK, CAP, 2))(specialist_choice_ids_keys, specialist_choice_ids_turns).reshape((SEQ, TOPK))
    cluster_chance = jnp.clip(0.1 + 0.5 * jax.random.uniform(streams_of[14], (SEQ,), jnp.float32) ** steps_of(streams_of[14], (SEQ,), ((0, 8),), -0.2, 0.2), 0.1, 0.6)
    specialist_duo_scores = scatter_about(streams_of[15], (SEQ, TOPK), 0.5, 2.0, ((0, 8),), jnp.float32)
    return dict(skip_path_vectors=skip_path_vectors, asker_raw_scores=asker_raw_scores, retain_raw_scores=retain_raw_scores, memory_write_entries=memory_write_entries, emit_switch_scores=emit_switch_scores, retain_minimum_share=retain_minimum_share, extra_shrink_rate=extra_shrink_rate, lane_rescale_factor=lane_rescale_factor, emit_projection_array=emit_projection_array, specialist_rescale_factor=specialist_rescale_factor, specialist_switch_proj=specialist_switch_proj, specialist_raise_proj=specialist_raise_proj, specialist_lower_proj=specialist_lower_proj, specialist_choice_ids=specialist_choice_ids, cluster_chance=cluster_chance, specialist_duo_scores=specialist_duo_scores)


EPS = 1e-06
PRECISE = lax.Precision.HIGHEST

def recurrence(queries, key_rows, values, shrink_log_rate):
    token_count_total = queries.shape[0]
    span_len = 64
    span_count = token_count_total // span_len
    causal = (jnp.arange(span_len)[:, None] >= jnp.arange(span_len)[None, :])[:, :, None, None]

    def advance(carried, inputs):
        query_span, key_span, value_span, decay_span = inputs
        cumulative = jnp.cumsum(decay_span, axis=0)
        spread = cumulative[:, None] - cumulative[None, :]
        factor = jnp.exp(jnp.where(causal, spread, -jnp.inf))
        scores = jnp.einsum('thd,shd,tshd->hts', query_span, key_span, factor, precision=PRECISE)
        inside = jnp.einsum('hts,shv->thv', scores, value_span, precision=PRECISE)
        outside = jnp.einsum('thd,hdv->thv', query_span * jnp.exp(cumulative), carried, precision=PRECISE)
        final_cum = cumulative[-1]
        written = jnp.einsum('shd,shv->hdv', key_span * jnp.exp(final_cum[None] - cumulative), value_span, precision=PRECISE)
        carried = jnp.exp(final_cum)[:, :, None] * carried + written
        return (carried, inside + outside)

    def split_spans(array):
        return array.reshape(span_count, span_len, SCAN_LANE_COUNT, KEY_WIDTH_SIZE)
    initial = jnp.zeros((SCAN_LANE_COUNT, KEY_WIDTH_SIZE, KEY_WIDTH_SIZE), jnp.float32)
    finished, output = lax.scan(advance, initial, tuple((split_spans(a) for a in (queries, key_rows, values, shrink_log_rate))))
    return output.reshape(token_count_total, SCAN_LANE_COUNT, KEY_WIDTH_SIZE)

def split_sum(left, right, groups):
    group_width = left.shape[1] // groups

    def add_group(running, group_idx):
        part_left = lax.dynamic_slice_in_dim(left, group_idx * group_width, group_width, 1)
        part_right = lax.dynamic_slice_in_dim(right, group_idx * group_width, group_width, 0)
        piece_sum = jnp.dot(part_left, part_right, preferred_element_type=jnp.float32)
        piece_sum = lax.optimization_barrier(piece_sum.astype(jnp.bfloat16)).astype(jnp.float32)
        return (running + piece_sum, None)
    zeros = jnp.zeros((left.shape[0], right.shape[1]), jnp.float32)
    total, finished = lax.scan(add_group, zeros, jnp.arange(groups, dtype=jnp.int32))
    return total

def experts_apply(normed, specialist_choice_ids, flat_weights, specialist_switch_proj, specialist_raise_proj, specialist_lower_proj):
    top_count = specialist_choice_ids.shape[1]
    flat_ids = specialist_choice_ids.reshape(-1)
    slot_limit = N_SP * CAP

    def one_expert(running, expert):
        ordering = jnp.argsort((flat_ids != expert).astype(jnp.int32), stable=True)[:slot_limit].astype(jnp.int32)
        chosen = flat_ids[ordering] == expert
        token_idx = (ordering // top_count).astype(jnp.int32)
        routed_rows = normed[token_idx]
        gate_acts = jnp.dot(routed_rows, specialist_switch_proj[expert], preferred_element_type=jnp.float32)
        up_acts = jnp.dot(routed_rows, specialist_raise_proj[expert], preferred_element_type=jnp.float32)
        hidden = (jax.nn.silu(gate_acts) * up_acts).astype(jnp.bfloat16)
        out_rows = split_sum(hidden, specialist_lower_proj[expert], N_TP).astype(jnp.bfloat16)
        scaled = jnp.where(chosen, flat_weights[ordering], 0.0)[:, None] * out_rows.astype(jnp.float32)
        return (running.at[token_idx].add(scaled), None)
    zeros = jnp.zeros(normed.shape, jnp.float32)
    total, finished = lax.scan(one_expert, zeros, jnp.arange(EXPERTS, dtype=jnp.int32))
    return total

def reference(skip_path_vectors, asker_raw_scores, retain_raw_scores, memory_write_entries, emit_switch_scores, retain_minimum_share, extra_shrink_rate, lane_rescale_factor, emit_projection_array, specialist_rescale_factor, specialist_switch_proj, specialist_raise_proj, specialist_lower_proj, specialist_choice_ids, cluster_chance, specialist_duo_scores):
    token_count_total = skip_path_vectors.shape[0]
    retain_share = retain_minimum_share + (1.0 - retain_minimum_share) * jax.nn.sigmoid(retain_raw_scores.astype(jnp.float32))
    shrink_log_rate = jnp.log(retain_share).reshape(token_count_total, SCAN_LANE_COUNT, KEY_WIDTH_SIZE) + extra_shrink_rate.T[:, :, None]
    key_rows = (1.0 - retain_share).reshape(token_count_total, SCAN_LANE_COUNT, KEY_WIDTH_SIZE)
    queries = jax.nn.silu(asker_raw_scores.astype(jnp.float32)).reshape(token_count_total, SCAN_LANE_COUNT, KEY_WIDTH_SIZE)
    values = memory_write_entries.astype(jnp.float32).reshape(token_count_total, SCAN_LANE_COUNT, KEY_WIDTH_SIZE)
    readout = recurrence(queries, key_rows, values, shrink_log_rate)
    normed_heads = readout * lax.rsqrt(lax.optimization_barrier(jnp.mean(readout * readout, axis=-1, keepdims=True)) + EPS)
    gated_out = normed_heads * lane_rescale_factor * jax.nn.silu(emit_switch_scores.astype(jnp.float32).reshape(token_count_total, SCAN_LANE_COUNT, KEY_WIDTH_SIZE))
    mixer_out = gated_out.reshape(token_count_total, SCAN_LANE_COUNT * KEY_WIDTH_SIZE).astype(jnp.bfloat16)
    resid = (skip_path_vectors.astype(jnp.float32) + split_sum(mixer_out, emit_projection_array, N_TP)).astype(jnp.bfloat16)
    wide_rows = resid.astype(jnp.float32)
    normed = (wide_rows * lax.rsqrt(lax.optimization_barrier(jnp.mean(wide_rows * wide_rows, axis=1, keepdims=True)) + EPS) * specialist_rescale_factor).astype(jnp.bfloat16)
    spread_logit = specialist_duo_scores[:, 0] - specialist_duo_scores[:, 1]
    weights = cluster_chance[:, None] * jnp.stack([jax.nn.sigmoid(spread_logit), jax.nn.sigmoid(-spread_logit)], axis=1)
    routed = experts_apply(normed, specialist_choice_ids, weights.reshape(-1), specialist_switch_proj, specialist_raise_proj, specialist_lower_proj)
    return (wide_rows + routed).astype(jnp.bfloat16)
```

```python
import functools

import jax
import jax.numpy as jnp
from jax import lax
from jax.experimental import pallas as pl
from jax.experimental.pallas import tpu as pltpu
from jax.sharding import PartitionSpec as P

EPS = 1e-06
PRECISE = lax.Precision.HIGHEST


MESH = pl.DeviceIdType.MESH
VMEM = pl.BlockSpec(memory_space=pltpu.VMEM)
VMEM_LIMIT = 60 * 1024 * 1024


def each(first, last, body):
    if last - first <= 8:
        for i in range(first, last):
            body(i)
    else:

        @pl.loop(first, last)
        def _(i):
            body(i)


def push(src, dst, send_sem, recv_sem, peer):
    return pltpu.make_async_remote_copy(
        src_ref=src,
        dst_ref=dst,
        send_sem=send_sem,
        recv_sem=recv_sem,
        device_id=peer,
        device_id_type=MESH,
    )


def state_kernel(sp_size, own_ref, out_ref, far_send, far_recv, near_send, near_recv):
    me = lax.axis_index("sp")
    pairs = sp_size // 2
    partner = me + 1 - 2 * lax.rem(me, 2)
    barrier = pltpu.get_barrier_semaphore()
    pl.semaphore_signal(barrier, inc=1, device_id={"sp": partner}, device_id_type=MESH)

    def far(d):
        return lax.rem(me + 2 * d, sp_size)

    def source(d):
        return lax.rem(me + sp_size - 2 * d, sp_size)

    def far_copy(d):
        return push(own_ref, out_ref.at[me], far_send.at[d], far_recv.at[d], {"sp": far(d)})

    def near_copy(d):
        block = own_ref if d is None else out_ref.at[source(d)]
        place = me if d is None else source(d)
        slot = 0 if d is None else d
        return push(
            block, out_ref.at[place], near_send.at[slot], near_recv.at[slot], {"sp": partner}
        )

    each(
        1,
        pairs,
        lambda d: pl.semaphore_signal(
            barrier, inc=1, device_id={"sp": far(d)}, device_id_type=MESH
        ),
    )
    pl.semaphore_wait(barrier, pairs)
    each(1, pairs, lambda d: far_copy(d).start())
    near_copy(None).start()

    def relay(d):
        far_copy(d).wait_recv()
        near_copy(d).start()

    each(1, pairs, relay)
    out_ref[me] = own_ref[...]
    near_copy(None).wait()

    def finish(d):
        far_copy(d).wait_send()
        near_copy(d).wait()

    each(1, pairs, finish)


def gather_states(packed):
    sp_size = lax.axis_size("sp")
    pairs = sp_size // 2
    dma = pltpu.SemaphoreType.DMA((pairs,))
    return pl.pallas_call(
        functools.partial(state_kernel, sp_size),
        out_shape=jax.ShapeDtypeStruct((sp_size,) + packed.shape, packed.dtype),
        in_specs=[VMEM],
        out_specs=VMEM,
        scratch_shapes=[dma, dma, dma, dma],
        compiler_params=pltpu.CompilerParams(collective_id=0, has_side_effects=True),
    )(packed)


def expert_kernel(
    sp_size,
    tp_size,
    group,
    mixer_ref,
    proj_ref,
    skip_ref,
    gain_ref,
    places_ref,
    gate_hbm,
    up_hbm,
    down_hbm,
    ret_ref,
    resid_ref,
    gate_w,
    up_w,
    down_w,
    pj,
    pj_in,
    sq,
    slots_in,
    slots,
    arr,
    part,
    got,
    hid,
    total,
    load_sem,
    pj_send,
    pj_recv,
    sq_send,
    sq_recv,
    out_send,
    out_recv,
    ag_send,
    ag_recv,
    rs_send,
    rs_recv,
    back_send,
    back_recv,
):
    my_s = lax.axis_index("sp")
    my_t = lax.axis_index("tp")
    tokens, width = skip_ref.shape
    cap = slots.shape[1]
    hidden_width = gate_w.shape[1]
    model_width = gate_w.shape[0]
    groups = sp_size // group
    rows = group * cap

    loads = [
        pltpu.make_async_copy(src, dst, load_sem.at[i])
        for i, (src, dst) in enumerate(((gate_hbm, gate_w), (up_hbm, up_w), (down_hbm, down_w)))
    ]
    barrier = pltpu.get_barrier_semaphore()

    def tp_of(j):
        return lax.rem(my_t + j, tp_size)

    def tp_from(j):
        return lax.rem(my_t + tp_size - j, tp_size)

    def sp_of(k):
        return lax.rem(my_s + k, sp_size)

    def sp_from(k):
        return lax.rem(my_s + sp_size - k, sp_size)

    each(
        1,
        tp_size,
        lambda j: pl.semaphore_signal(barrier, inc=1, device_id={"tp": tp_of(j)}, device_id_type=MESH),
    )
    each(
        1,
        sp_size,
        lambda k: pl.semaphore_signal(barrier, inc=1, device_id={"sp": sp_of(k)}, device_id_type=MESH),
    )
    for load in loads:
        load.start()

    def project(t):
        cols = pl.ds(pl.multiple_of(t * width, width), width)
        return jnp.dot(mixer_ref[...], proj_ref[:, cols], preferred_element_type=jnp.float32).astype(
            jnp.bfloat16
        )

    def pj_copy(j):
        return push(pj.at[j], pj_in.at[j], pj_send.at[j], pj_recv.at[j], {"tp": tp_of(j)})

    def project_all(j):
        pj[j] = project(tp_of(j))

    each(1, tp_size, project_all)
    pl.semaphore_wait(barrier, tp_size + sp_size - 2)
    each(1, tp_size, lambda j: pj_copy(j).start())
    total[...] = project(my_t).astype(jnp.float32)

    def add_in(j):
        pj_copy(j).wait_recv()
        total[...] += pj_in[j].astype(jnp.float32)

    each(1, tp_size, add_in)
    resid = (skip_ref[...].astype(jnp.float32) + total[...]).astype(jnp.bfloat16)
    resid_ref[...] = resid
    wide = resid.astype(jnp.float32)
    row_sums = jnp.sum(wide * wide, axis=1, keepdims=True)
    sq[0] = jnp.transpose(jnp.broadcast_to(row_sums, (tokens, 128)))[:8]

    def sq_copy(j):
        return push(sq.at[0], sq.at[j], sq_send.at[j], sq_recv.at[j], {"tp": tp_of(j)})

    each(1, tp_size, lambda j: sq_copy(j).start())
    slot_ids = lax.broadcasted_iota(jnp.int32, (sp_size * cap, tokens), 0)
    chosen = (slot_ids == places_ref[0:1, :]) | (slot_ids == places_ref[1:2, :])
    one_hot = chosen.astype(jnp.float32).astype(jnp.bfloat16)
    each(1, tp_size, lambda j: sq_copy(j).wait())
    squares = jnp.sum(sq[...], axis=0)[0:1]
    squares = jnp.transpose(jnp.broadcast_to(squares, (128, tokens)))[:, 0:1]
    normed = (wide * lax.rsqrt(squares / model_width + EPS) * gain_ref[...]).astype(jnp.bfloat16)
    filled = jnp.dot(one_hot, normed, preferred_element_type=jnp.float32).astype(jnp.bfloat16)
    slots_in[...] = filled.reshape(sp_size, cap, width)
    arr[my_t, 0] = filled[:cap]

    def out_copy(k):
        return push(
            slots_in.at[k], arr.at[my_t, k], out_send.at[k], out_recv.at[k], {"sp": sp_of(k)}
        )

    each(1, sp_size, lambda k: out_copy(k).start())

    def span(g):
        return pl.ds(g * group, group)

    def ag_copy(g, j):
        block = arr.at[my_t, span(g)]
        return push(block, block, ag_send.at[j, g], ag_recv.at[j, g], {"tp": tp_of(j)})

    def rs_copy(g, j):
        return push(
            part.at[j, span(g)],
            got.at[j, span(g)],
            rs_send.at[j, g],
            rs_recv.at[j, g],
            {"tp": tp_of(j)},
        )

    def back_copy(k):
        return push(
            slots.at[k], ret_ref.at[k], back_send.at[k], back_recv.at[k], {"sp": sp_from(k)}
        )


    def dispatch(g):
        def take(i):
            out_copy(g * group + i).wait_recv()

        each(1 if isinstance(g, int) and g == 0 else 0, group, take)
        each(1, tp_size, lambda j: ag_copy(g, j).start())

    dispatch(0)
    each(1, groups, dispatch)
    for load in loads:
        load.wait()
    tile = min(256, hidden_width)

    @pl.loop(0, groups)
    def _(g):
        each(1, tp_size, lambda j: ag_copy(g, j).wait_recv())

        @pl.loop(0, hidden_width // tile)
        def _(f):
            cols = pl.ds(pl.multiple_of(f * tile, tile), tile)
            gate = jnp.zeros((rows, tile), jnp.float32)
            up = jnp.zeros((rows, tile), jnp.float32)
            for t in range(tp_size):
                x = arr[t, span(g)].reshape(rows, width)
                depth = slice(t * width, (t + 1) * width)
                gate += jnp.dot(x, gate_w[depth, cols], preferred_element_type=jnp.float32)
                up += jnp.dot(x, up_w[depth, cols], preferred_element_type=jnp.float32)
            hid[:, cols] = (gate * jax.nn.sigmoid(gate) * up).astype(jnp.bfloat16)

        def lower(j):
            cols = pl.ds(pl.multiple_of(tp_of(j) * width, width), width)
            out = jnp.dot(hid[...], down_w[:, cols], preferred_element_type=jnp.float32)
            part[j, span(g)] = out.astype(jnp.bfloat16).reshape(group, cap, width)

        each(1, tp_size, lower)
        each(1, tp_size, lambda j: rs_copy(g, j).start())
        lower(0)

    def give_back(g):
        acc = part[0, span(g)].astype(jnp.float32)
        for j in range(1, tp_size):
            rs_copy(g, j).wait_recv()
            acc += got[j, span(g)].astype(jnp.float32)
        slots[span(g)] = acc.astype(jnp.bfloat16)
        each(
            1 if isinstance(g, int) and g == 0 else 0,
            group,
            lambda i: back_copy(g * group + i).start(),
        )

    give_back(0)
    each(1, groups, give_back)
    ret_ref[0] = slots[0]
    each(1, sp_size, lambda k: back_copy(k).wait())
    each(1, sp_size, lambda k: out_copy(k).wait_send())

    def drain(j):
        pj_copy(j).wait_send()
        for g in range(groups):
            ag_copy(g, j).wait_send()
            rs_copy(g, j).wait_send()

    each(1, tp_size, drain)


def run_experts(mixer_out, projection, skip_cols, gain_cols, places, gate, up, down, cap):
    sp_size = lax.axis_size("sp")
    tp_size = lax.axis_size("tp")
    tokens, width = skip_cols.shape
    model_width, hidden_width = gate.shape
    group = max(g for g in range(1, sp_size + 1) if sp_size % g == 0 and g * cap <= 256)
    groups = sp_size // group
    bf, f32 = jnp.bfloat16, jnp.float32
    dma = pltpu.SemaphoreType.DMA
    anywhere = pl.BlockSpec(memory_space=pl.ANY)
    return pl.pallas_call(
        functools.partial(expert_kernel, sp_size, tp_size, group),
        out_shape=(
            jax.ShapeDtypeStruct((sp_size, cap, width), bf),
            jax.ShapeDtypeStruct((tokens, width), bf),
        ),
        in_specs=[VMEM] * 5 + [anywhere] * 3,
        out_specs=(VMEM, VMEM),
        scratch_shapes=[
            pltpu.VMEM((model_width, hidden_width), bf),
            pltpu.VMEM((model_width, hidden_width), bf),
            pltpu.VMEM((hidden_width, model_width), bf),
            pltpu.VMEM((tp_size, tokens, width), bf),
            pltpu.VMEM((tp_size, tokens, width), bf),
            pltpu.VMEM((tp_size, 8, tokens), f32),
            pltpu.VMEM((sp_size, cap, width), bf),
            pltpu.VMEM((sp_size, cap, width), bf),
            pltpu.VMEM((tp_size, sp_size, cap, width), bf),
            pltpu.VMEM((tp_size, sp_size, cap, width), bf),
            pltpu.VMEM((tp_size, sp_size, cap, width), bf),
            pltpu.VMEM((group * cap, hidden_width), bf),
            pltpu.VMEM((tokens, width), f32),
            dma((3,)),
            dma((tp_size,)),
            dma((tp_size,)),
            dma((tp_size,)),
            dma((tp_size,)),
            dma((sp_size,)),
            dma((sp_size,)),
            dma((tp_size, groups)),
            dma((tp_size, groups)),
            dma((tp_size, groups)),
            dma((tp_size, groups)),
            dma((sp_size,)),
            dma((sp_size,)),
        ],
        compiler_params=pltpu.CompilerParams(
            collective_id=1, has_side_effects=True, vmem_limit_bytes=VMEM_LIMIT
        ),
    )(mixer_out, projection, skip_cols, gain_cols, places, gate, up, down)


def carry_states(totals, own_state):
    lanes, depth = totals.shape
    sp_size = lax.axis_size("sp")
    place = lax.axis_index("sp")
    pad = -lanes % 16
    packed = jnp.concatenate(
        [
            own_state.astype(jnp.bfloat16).reshape(lanes * depth, depth),
            totals.astype(jnp.bfloat16),
            jnp.zeros((pad, depth), jnp.bfloat16),
        ]
    )
    gathered = gather_states(packed)
    states = gathered[:, : lanes * depth].reshape(sp_size, lanes, depth, depth)
    shrinks = gathered[:, lanes * depth : lanes * depth + lanes].astype(jnp.float32)
    factor = jnp.ones((lanes, depth), jnp.float32)
    carried = jnp.zeros((lanes, depth, depth), jnp.float32)
    for lap in reversed(range(sp_size)):
        earlier = lap < place
        held = states[lap].astype(jnp.float32) * factor[:, :, None]
        carried = carried + jnp.where(earlier, held, 0.0)
        factor = jnp.where(earlier, factor * shrinks[lap], factor)
    return carried


def shards(
    skip_path_vectors,
    asker_raw_scores,
    retain_raw_scores,
    memory_write_entries,
    emit_switch_scores,
    retain_minimum_share,
    extra_shrink_rate,
    lane_rescale_factor,
    emit_projection_array,
    specialist_rescale_factor,
    specialist_switch_proj,
    specialist_raise_proj,
    specialist_lower_proj,
    specialist_choice_ids,
    cluster_chance,
    specialist_duo_scores,
):
    token_count_total = skip_path_vectors.shape[0]
    model_width = skip_path_vectors.shape[1]
    head_depth = lane_rescale_factor.shape[0]
    lanes_on_device = extra_shrink_rate.shape[0]
    retain_share = retain_minimum_share + (1.0 - retain_minimum_share) * jax.nn.sigmoid(
        retain_raw_scores.astype(jnp.float32)
    )
    retain_share = retain_share.reshape(token_count_total, lanes_on_device, head_depth)
    shrink_log_rate = jnp.log(retain_share) + extra_shrink_rate.T[:, :, None]
    key_rows = 1.0 - retain_share
    queries = jax.nn.silu(asker_raw_scores.astype(jnp.float32)).reshape(
        token_count_total, lanes_on_device, head_depth
    )
    values = memory_write_entries.astype(jnp.float32).reshape(
        token_count_total, lanes_on_device, head_depth
    )
    cumulative = jnp.cumsum(shrink_log_rate, axis=0)
    query_tilde = queries * jnp.exp(cumulative)
    key_tilde = key_rows * jnp.exp(-cumulative)
    causal = jnp.arange(token_count_total)[:, None] >= jnp.arange(token_count_total)[None, :]
    scores = jnp.einsum("thd,shd->hts", query_tilde, key_tilde, precision=PRECISE)
    scores = jnp.where(causal[None], scores, 0.0)
    inside = jnp.einsum("hts,shv->thv", scores, values, precision=PRECISE)
    totals = jnp.exp(cumulative[-1])
    own_state = jnp.einsum("shd,shv->hdv", key_tilde * totals[None], values, precision=PRECISE)
    carried = carry_states(totals, own_state)
    outside = jnp.einsum("thd,hdv->thv", query_tilde, carried, precision=PRECISE)
    readout = inside + outside
    normed_heads = readout * lax.rsqrt(jnp.mean(readout * readout, axis=-1, keepdims=True) + EPS)
    gated_out = (
        normed_heads
        * lane_rescale_factor
        * jax.nn.silu(
            emit_switch_scores.astype(jnp.float32).reshape(
                token_count_total, lanes_on_device, head_depth
            )
        )
    )
    mixer_out = gated_out.reshape(token_count_total, lanes_on_device * head_depth).astype(
        jnp.bfloat16
    )
    tp_size = lax.axis_size("tp")
    sp_size = lax.axis_size("sp")
    experts = sp_size
    top_count = specialist_choice_ids.shape[1]
    capacity = -(-3 * token_count_total * top_count // (2 * experts))
    capacity = -(-capacity // 16) * 16
    flat_ids = specialist_choice_ids.reshape(-1)
    matches = (flat_ids[:, None] == jnp.arange(experts, dtype=jnp.int32)[None, :]).astype(jnp.int32)
    before = jnp.cumsum(matches, axis=0) - matches
    turn = lax.rem(flat_ids + sp_size - lax.axis_index("sp"), sp_size)
    places = turn * capacity + jnp.sum(before * matches, axis=1)
    places = places.reshape(token_count_total, top_count)
    col_width = model_width // tp_size
    col_start = lax.axis_index("tp") * col_width
    skip_cols = lax.dynamic_slice_in_dim(skip_path_vectors, col_start, col_width, 1)
    gain_cols = lax.dynamic_slice_in_dim(specialist_rescale_factor, col_start, col_width, 0)
    returned, resid_cols = run_experts(
        mixer_out,
        emit_projection_array,
        skip_cols,
        gain_cols[None, :],
        places.T,
        specialist_switch_proj[0],
        specialist_raise_proj[0],
        specialist_lower_proj[0],
        capacity,
    )
    returned = returned.reshape(sp_size * capacity, col_width)
    slot_ids = jnp.arange(sp_size * capacity, dtype=jnp.int32)[None, :]
    picked = jnp.stack(
        [
            jnp.dot(
                (places[:, j : j + 1] == slot_ids).astype(jnp.bfloat16),
                returned,
                preferred_element_type=jnp.float32,
            )
            for j in range(top_count)
        ],
        axis=1,
    )
    spread_logit = specialist_duo_scores[:, 0] - specialist_duo_scores[:, 1]
    weights = cluster_chance[:, None] * jnp.stack(
        [jax.nn.sigmoid(spread_logit), jax.nn.sigmoid(-spread_logit)], axis=1
    )
    mixed_out = resid_cols.astype(jnp.float32) + jnp.sum(
        weights[:, :, None] * picked.astype(jnp.float32), axis=1
    )
    return mixed_out.astype(jnp.bfloat16)


def solution(mesh):
    return jax.shard_map(
        shards,
        mesh=mesh,
        in_specs=(
            P("sp", None),
            P("sp", "tp"),
            P("sp", "tp"),
            P("sp", "tp"),
            P("sp", "tp"),
            P("tp"),
            P("tp", "sp"),
            P(),
            P("tp", None),
            P(),
            P("sp", None, "tp"),
            P("sp", None, "tp"),
            P("sp", "tp", None),
            P("sp", None),
            P("sp"),
            P("sp", None),
        ),
        out_specs=P("sp", "tp"),
        check_vma=False,
    )
```

```python
import functools

import jax
import jax.numpy as jnp
from jax import lax
from jax.experimental import pallas as pl
from jax.experimental.pallas import tpu as pltpu
from jax.sharding import PartitionSpec as P

EPS = 1e-06
PRECISE = lax.Precision.HIGHEST


MESH = pl.DeviceIdType.MESH
VMEM = pl.BlockSpec(memory_space=pltpu.VMEM)
VMEM_LIMIT = 60 * 1024 * 1024


def each(first, last, body):
    if last - first <= 8:
        for i in range(first, last):
            body(i)
    else:

        @pl.loop(first, last)
        def _(i):
            body(i)


def push(src, dst, send_sem, recv_sem, peer):
    return pltpu.make_async_remote_copy(
        src_ref=src,
        dst_ref=dst,
        send_sem=send_sem,
        recv_sem=recv_sem,
        device_id=peer,
        device_id_type=MESH,
    )


def state_kernel(sp_size, own_ref, out_ref, far_send, far_recv, near_send, near_recv):
    me = lax.axis_index("sp")
    pairs = sp_size // 2
    partner = me + 1 - 2 * lax.rem(me, 2)
    barrier = pltpu.get_barrier_semaphore()
    pl.semaphore_signal(barrier, inc=1, device_id={"sp": partner}, device_id_type=MESH)

    def far(d):
        return lax.rem(me + 2 * d, sp_size)

    def source(d):
        return lax.rem(me + sp_size - 2 * d, sp_size)

    def far_copy(d):
        return push(own_ref, out_ref.at[me], far_send.at[d], far_recv.at[d], {"sp": far(d)})

    def near_copy(d):
        block = own_ref if d is None else out_ref.at[source(d)]
        place = me if d is None else source(d)
        slot = 0 if d is None else d
        return push(
            block, out_ref.at[place], near_send.at[slot], near_recv.at[slot], {"sp": partner}
        )

    each(
        1,
        pairs,
        lambda d: pl.semaphore_signal(
            barrier, inc=1, device_id={"sp": far(d)}, device_id_type=MESH
        ),
    )
    pl.semaphore_wait(barrier, pairs)
    each(1, pairs, lambda d: far_copy(d).start())
    near_copy(None).start()

    def relay(d):
        far_copy(d).wait_recv()
        near_copy(d).start()

    each(1, pairs, relay)
    out_ref[me] = own_ref[...]
    near_copy(None).wait()

    def finish(d):
        far_copy(d).wait_send()
        near_copy(d).wait()

    each(1, pairs, finish)


def gather_states(packed):
    sp_size = lax.axis_size("sp")
    pairs = sp_size // 2
    dma = pltpu.SemaphoreType.DMA((pairs,))
    return pl.pallas_call(
        functools.partial(state_kernel, sp_size),
        out_shape=jax.ShapeDtypeStruct((sp_size,) + packed.shape, packed.dtype),
        in_specs=[VMEM],
        out_specs=VMEM,
        scratch_shapes=[dma, dma, dma, dma],
        compiler_params=pltpu.CompilerParams(collective_id=0, has_side_effects=True),
    )(packed)


def expert_kernel(
    sp_size,
    tp_size,
    group,
    mixer_ref,
    proj_ref,
    skip_ref,
    gain_ref,
    places_ref,
    gate_hbm,
    up_hbm,
    down_hbm,
    ret_ref,
    resid_ref,
    gate_w,
    up_w,
    down_w,
    pj,
    pj_in,
    sq,
    slots_in,
    slots,
    arr,
    part,
    got,
    hid,
    total,
    load_sem,
    pj_send,
    pj_recv,
    sq_send,
    sq_recv,
    out_send,
    out_recv,
    ag_send,
    ag_recv,
    rs_send,
    rs_recv,
    back_send,
    back_recv,
):
    my_s = lax.axis_index("sp")
    my_t = lax.axis_index("tp")
    tokens, width = skip_ref.shape
    cap = slots.shape[1]
    hidden_width = gate_w.shape[1]
    model_width = gate_w.shape[0]
    groups = sp_size // group
    rows = group * cap

    loads = [
        pltpu.make_async_copy(src, dst, load_sem.at[i])
        for i, (src, dst) in enumerate(((gate_hbm, gate_w), (up_hbm, up_w), (down_hbm, down_w)))
    ]
    barrier = pltpu.get_barrier_semaphore()

    square = tp_size == 4 and group % 2 == 0

    def tp_of(j):
        if not square:
            return lax.rem(my_t + j, tp_size)
        return (my_t, my_t + 1 - 2 * lax.rem(my_t, 2), lax.rem(my_t + 2, 4), 3 - my_t)[j]

    def sp_of(k):
        return lax.rem(my_s + k, sp_size)

    def sp_from(k):
        return lax.rem(my_s + sp_size - k, sp_size)

    each(
        1,
        tp_size,
        lambda j: pl.semaphore_signal(barrier, inc=1, device_id={"tp": tp_of(j)}, device_id_type=MESH),
    )
    each(
        1,
        sp_size,
        lambda k: pl.semaphore_signal(barrier, inc=1, device_id={"sp": sp_of(k)}, device_id_type=MESH),
    )
    for load in loads:
        load.start()

    def project(t):
        cols = pl.ds(pl.multiple_of(t * width, width), width)
        return jnp.dot(mixer_ref[...], proj_ref[:, cols], preferred_element_type=jnp.float32).astype(
            jnp.bfloat16
        )

    def pj_copy(j):
        return push(pj.at[j], pj_in.at[j], pj_send.at[j], pj_recv.at[j], {"tp": tp_of(j)})

    def project_all(j):
        pj[j] = project(tp_of(j))

    each(1, tp_size, project_all)
    pl.semaphore_wait(barrier, tp_size + sp_size - 2)
    each(1, tp_size, lambda j: pj_copy(j).start())
    total[...] = project(my_t).astype(jnp.float32)

    def add_in(j):
        pj_copy(j).wait_recv()
        total[...] += pj_in[j].astype(jnp.float32)

    each(1, tp_size, add_in)
    resid = (skip_ref[...].astype(jnp.float32) + total[...]).astype(jnp.bfloat16)
    resid_ref[...] = resid
    wide = resid.astype(jnp.float32)
    row_sums = jnp.sum(wide * wide, axis=1, keepdims=True)
    sq[0] = jnp.transpose(jnp.broadcast_to(row_sums, (tokens, 128)))[:8]

    def sq_copy(j):
        return push(sq.at[0], sq.at[j], sq_send.at[j], sq_recv.at[j], {"tp": tp_of(j)})

    each(1, tp_size, lambda j: sq_copy(j).start())
    slot_ids = lax.broadcasted_iota(jnp.int32, (sp_size * cap, tokens), 0)
    chosen = (slot_ids == places_ref[0:1, :]) | (slot_ids == places_ref[1:2, :])
    one_hot = chosen.astype(jnp.float32).astype(jnp.bfloat16)
    each(1, tp_size, lambda j: sq_copy(j).wait())
    squares = jnp.sum(sq[...], axis=0)[0:1]
    squares = jnp.transpose(jnp.broadcast_to(squares, (128, tokens)))[:, 0:1]
    normed = (wide * lax.rsqrt(squares / model_width + EPS) * gain_ref[...]).astype(jnp.bfloat16)
    filled = jnp.dot(one_hot, normed, preferred_element_type=jnp.float32).astype(jnp.bfloat16)
    slots_in[...] = filled.reshape(sp_size, cap, width)
    arr[my_t, 0] = filled[:cap]

    def out_copy(k):
        return push(
            slots_in.at[k], arr.at[my_t, k], out_send.at[k], out_recv.at[k], {"sp": sp_of(k)}
        )

    each(1, sp_size, lambda k: out_copy(k).start())

    def span(g):
        return pl.ds(g * group, group)

    def ag_copy(g, j):
        block = arr.at[my_t, span(g)]
        return push(block, block, ag_send.at[j, g], ag_recv.at[j, g], {"tp": tp_of(j)})

    def rs_copy(g, j):
        return push(
            part.at[j, span(g)],
            got.at[j, span(g)],
            rs_send.at[j, g],
            rs_recv.at[j, g],
            {"tp": tp_of(j)},
        )

    def back_copy(k):
        return push(
            slots.at[k], ret_ref.at[k], back_send.at[k], back_recv.at[k], {"sp": sp_from(k)}
        )


    ag_peers = 3 if square else tp_size
    half = group // 2

    def relays(g):
        first = arr.at[tp_of(1), pl.ds(g * group, half)]
        second = arr.at[tp_of(2), pl.ds(g * group + half, half)]
        return (
            push(first, first, ag_send.at[3, g], ag_recv.at[3, g], {"tp": tp_of(2)}),
            push(second, second, ag_send.at[0, g], ag_recv.at[0, g], {"tp": tp_of(1)}),
        )

    def relay(g):
        for j, copy in zip((1, 2), relays(g)):
            ag_copy(g, j).wait_recv()
            copy.start()

    def dispatch(g):
        def take(i):
            out_copy(g * group + i).wait_recv()

        each(1 if isinstance(g, int) and g == 0 else 0, group, take)
        each(1, ag_peers, lambda j: ag_copy(g, j).start())

    dispatch(0)
    each(1, groups, dispatch)
    for load in loads:
        load.wait()
    tile = min(256, hidden_width)

    ahead = min(2, groups)
    if square:
        for g in range(ahead):
            relay(g)

    @pl.loop(0, groups)
    def _(g):
        if square:

            @pl.when(g + ahead < groups)
            def _():
                relay(g + ahead)

            for copy in relays(g):
                copy.wait_recv()
        else:
            each(1, tp_size, lambda j: ag_copy(g, j).wait_recv())

        @pl.loop(0, hidden_width // tile)
        def _(f):
            cols = pl.ds(pl.multiple_of(f * tile, tile), tile)
            gate = jnp.zeros((rows, tile), jnp.float32)
            up = jnp.zeros((rows, tile), jnp.float32)
            for t in range(tp_size):
                x = arr[t, span(g)].reshape(rows, width)
                depth = slice(t * width, (t + 1) * width)
                gate += jnp.dot(x, gate_w[depth, cols], preferred_element_type=jnp.float32)
                up += jnp.dot(x, up_w[depth, cols], preferred_element_type=jnp.float32)
            hid[:, cols] = (gate * jax.nn.sigmoid(gate) * up).astype(jnp.bfloat16)

        def lower(j):
            cols = pl.ds(pl.multiple_of(tp_of(j) * width, width), width)
            out = jnp.dot(hid[...], down_w[:, cols], preferred_element_type=jnp.float32)
            part[j, span(g)] = out.astype(jnp.bfloat16).reshape(group, cap, width)

        each(1, tp_size, lower)
        each(1, tp_size, lambda j: rs_copy(g, j).start())
        lower(0)

    def give_back(g):
        acc = part[0, span(g)].astype(jnp.float32)
        for j in range(1, tp_size):
            rs_copy(g, j).wait_recv()
            acc += got[j, span(g)].astype(jnp.float32)
        slots[span(g)] = acc.astype(jnp.bfloat16)
        each(
            1 if isinstance(g, int) and g == 0 else 0,
            group,
            lambda i: back_copy(g * group + i).start(),
        )

    give_back(0)
    each(1, groups, give_back)
    ret_ref[0] = slots[0]
    each(1, sp_size, lambda k: back_copy(k).wait())
    each(1, sp_size, lambda k: out_copy(k).wait_send())

    def drain(j):
        pj_copy(j).wait_send()
        for g in range(groups):
            rs_copy(g, j).wait_send()

    each(1, tp_size, drain)
    for g in range(groups):
        each(1, ag_peers, lambda j: ag_copy(g, j).wait_send())
        if square:
            for copy in relays(g):
                copy.wait_send()


def run_experts(mixer_out, projection, skip_cols, gain_cols, places, gate, up, down, cap):
    sp_size = lax.axis_size("sp")
    tp_size = lax.axis_size("tp")
    tokens, width = skip_cols.shape
    model_width, hidden_width = gate.shape
    group = max(g for g in range(1, sp_size + 1) if sp_size % g == 0 and g * cap <= 256)
    groups = sp_size // group
    bf, f32 = jnp.bfloat16, jnp.float32
    dma = pltpu.SemaphoreType.DMA
    anywhere = pl.BlockSpec(memory_space=pl.ANY)
    return pl.pallas_call(
        functools.partial(expert_kernel, sp_size, tp_size, group),
        out_shape=(
            jax.ShapeDtypeStruct((sp_size, cap, width), bf),
            jax.ShapeDtypeStruct((tokens, width), bf),
        ),
        in_specs=[VMEM] * 5 + [anywhere] * 3,
        out_specs=(VMEM, VMEM),
        scratch_shapes=[
            pltpu.VMEM((model_width, hidden_width), bf),
            pltpu.VMEM((model_width, hidden_width), bf),
            pltpu.VMEM((hidden_width, model_width), bf),
            pltpu.VMEM((tp_size, tokens, width), bf),
            pltpu.VMEM((tp_size, tokens, width), bf),
            pltpu.VMEM((tp_size, 8, tokens), f32),
            pltpu.VMEM((sp_size, cap, width), bf),
            pltpu.VMEM((sp_size, cap, width), bf),
            pltpu.VMEM((tp_size, sp_size, cap, width), bf),
            pltpu.VMEM((tp_size, sp_size, cap, width), bf),
            pltpu.VMEM((tp_size, sp_size, cap, width), bf),
            pltpu.VMEM((group * cap, hidden_width), bf),
            pltpu.VMEM((tokens, width), f32),
            dma((3,)),
            dma((tp_size,)),
            dma((tp_size,)),
            dma((tp_size,)),
            dma((tp_size,)),
            dma((sp_size,)),
            dma((sp_size,)),
            dma((tp_size, groups)),
            dma((tp_size, groups)),
            dma((tp_size, groups)),
            dma((tp_size, groups)),
            dma((sp_size,)),
            dma((sp_size,)),
        ],
        compiler_params=pltpu.CompilerParams(
            collective_id=1, has_side_effects=True, vmem_limit_bytes=VMEM_LIMIT
        ),
    )(mixer_out, projection, skip_cols, gain_cols, places, gate, up, down)


def carry_states(totals, own_state):
    lanes, depth = totals.shape
    sp_size = lax.axis_size("sp")
    place = lax.axis_index("sp")
    pad = -lanes % 16
    packed = jnp.concatenate(
        [
            own_state.astype(jnp.bfloat16).reshape(lanes * depth, depth),
            totals.astype(jnp.bfloat16),
            jnp.zeros((pad, depth), jnp.bfloat16),
        ]
    )
    gathered = gather_states(packed)
    states = gathered[:, : lanes * depth].reshape(sp_size, lanes, depth, depth)
    shrinks = gathered[:, lanes * depth : lanes * depth + lanes].astype(jnp.float32)
    factor = jnp.ones((lanes, depth), jnp.float32)
    carried = jnp.zeros((lanes, depth, depth), jnp.float32)
    for lap in reversed(range(sp_size)):
        earlier = lap < place
        held = states[lap].astype(jnp.float32) * factor[:, :, None]
        carried = carried + jnp.where(earlier, held, 0.0)
        factor = jnp.where(earlier, factor * shrinks[lap], factor)
    return carried


def shards(
    skip_path_vectors,
    asker_raw_scores,
    retain_raw_scores,
    memory_write_entries,
    emit_switch_scores,
    retain_minimum_share,
    extra_shrink_rate,
    lane_rescale_factor,
    emit_projection_array,
    specialist_rescale_factor,
    specialist_switch_proj,
    specialist_raise_proj,
    specialist_lower_proj,
    specialist_choice_ids,
    cluster_chance,
    specialist_duo_scores,
):
    token_count_total = skip_path_vectors.shape[0]
    model_width = skip_path_vectors.shape[1]
    head_depth = lane_rescale_factor.shape[0]
    lanes_on_device = extra_shrink_rate.shape[0]
    retain_share = retain_minimum_share + (1.0 - retain_minimum_share) * jax.nn.sigmoid(
        retain_raw_scores.astype(jnp.float32)
    )
    retain_share = retain_share.reshape(token_count_total, lanes_on_device, head_depth)
    shrink_log_rate = jnp.log(retain_share) + extra_shrink_rate.T[:, :, None]
    key_rows = 1.0 - retain_share
    queries = jax.nn.silu(asker_raw_scores.astype(jnp.float32)).reshape(
        token_count_total, lanes_on_device, head_depth
    )
    values = memory_write_entries.astype(jnp.float32).reshape(
        token_count_total, lanes_on_device, head_depth
    )
    cumulative = jnp.cumsum(shrink_log_rate, axis=0)
    query_tilde = queries * jnp.exp(cumulative)
    key_tilde = key_rows * jnp.exp(-cumulative)
    causal = jnp.arange(token_count_total)[:, None] >= jnp.arange(token_count_total)[None, :]
    scores = jnp.einsum("thd,shd->hts", query_tilde, key_tilde, precision=PRECISE)
    scores = jnp.where(causal[None], scores, 0.0)
    inside = jnp.einsum("hts,shv->thv", scores, values, precision=PRECISE)
    totals = jnp.exp(cumulative[-1])
    own_state = jnp.einsum("shd,shv->hdv", key_tilde * totals[None], values, precision=PRECISE)
    carried = carry_states(totals, own_state)
    outside = jnp.einsum("thd,hdv->thv", query_tilde, carried, precision=PRECISE)
    readout = inside + outside
    normed_heads = readout * lax.rsqrt(jnp.mean(readout * readout, axis=-1, keepdims=True) + EPS)
    gated_out = (
        normed_heads
        * lane_rescale_factor
        * jax.nn.silu(
            emit_switch_scores.astype(jnp.float32).reshape(
                token_count_total, lanes_on_device, head_depth
            )
        )
    )
    mixer_out = gated_out.reshape(token_count_total, lanes_on_device * head_depth).astype(
        jnp.bfloat16
    )
    tp_size = lax.axis_size("tp")
    sp_size = lax.axis_size("sp")
    experts = sp_size
    top_count = specialist_choice_ids.shape[1]
    capacity = -(-3 * token_count_total * top_count // (2 * experts))
    capacity = -(-capacity // 16) * 16
    flat_ids = specialist_choice_ids.reshape(-1)
    matches = (flat_ids[:, None] == jnp.arange(experts, dtype=jnp.int32)[None, :]).astype(jnp.int32)
    before = jnp.cumsum(matches, axis=0) - matches
    turn = lax.rem(flat_ids + sp_size - lax.axis_index("sp"), sp_size)
    places = turn * capacity + jnp.sum(before * matches, axis=1)
    places = places.reshape(token_count_total, top_count)
    col_width = model_width // tp_size
    col_start = lax.axis_index("tp") * col_width
    skip_cols = lax.dynamic_slice_in_dim(skip_path_vectors, col_start, col_width, 1)
    gain_cols = lax.dynamic_slice_in_dim(specialist_rescale_factor, col_start, col_width, 0)
    returned, resid_cols = run_experts(
        mixer_out,
        emit_projection_array,
        skip_cols,
        gain_cols[None, :],
        places.T,
        specialist_switch_proj[0],
        specialist_raise_proj[0],
        specialist_lower_proj[0],
        capacity,
    )
    returned = returned.reshape(sp_size * capacity, col_width)
    slot_ids = jnp.arange(sp_size * capacity, dtype=jnp.int32)[None, :]
    picked = jnp.stack(
        [
            jnp.dot(
                (places[:, j : j + 1] == slot_ids).astype(jnp.bfloat16),
                returned,
                preferred_element_type=jnp.float32,
            )
            for j in range(top_count)
        ],
        axis=1,
    )
    spread_logit = specialist_duo_scores[:, 0] - specialist_duo_scores[:, 1]
    weights = cluster_chance[:, None] * jnp.stack(
        [jax.nn.sigmoid(spread_logit), jax.nn.sigmoid(-spread_logit)], axis=1
    )
    mixed_out = resid_cols.astype(jnp.float32) + jnp.sum(
        weights[:, :, None] * picked.astype(jnp.float32), axis=1
    )
    return mixed_out.astype(jnp.bfloat16)


def solution(mesh):
    return jax.shard_map(
        shards,
        mesh=mesh,
        in_specs=(
            P("sp", None),
            P("sp", "tp"),
            P("sp", "tp"),
            P("sp", "tp"),
            P("sp", "tp"),
            P("tp"),
            P("tp", "sp"),
            P(),
            P("tp", None),
            P(),
            P("sp", None, "tp"),
            P("sp", None, "tp"),
            P("sp", "tp", None),
            P("sp", None),
            P("sp"),
            P("sp", None),
        ),
        out_specs=P("sp", "tp"),
        check_vma=False,
    )
```
